32 devices in a mesh: ep: 8 (over z, x), tp: 4 (over y, core).
Axes of the slice: x: 2, y: 2, z: 4, core: 2. Of those that a mesh axis runs over, the one named last changes fastest.
Arguments:
- queries: bfloat16 [8192, 2048], P('ep', 'tp'), may hold values from -6 to 6
- key_vectors: bfloat16 [8192, 2048], P('ep', 'tp'), may hold values from -6 to 6
- value_vectors: bfloat16 [8192, 4096], P('ep', 'tp'), may hold values from -6 to 6
- decay_logit: float32 [8192, 2048], P('ep', 'tp'), may hold values from -11 to 16
- head_gain: float32 [256], replicated, may hold values from 0.1 to 1.9
- routed_rows: bfloat16 [2048, 4096], P('ep'), may hold values from -6 to 6
- pre_gain: float32 [4096], replicated, may hold values from 0.1 to 1.9
- expert_pick: int32 [2048, 2], P('ep'), may hold values from 0 to 7, as said below
- route_weight: float32 [2048, 2], P('ep'), may hold values from 0.2 to 1
- gate_weight: bfloat16 [8, 4096, 2048], P('ep', None, 'tp'), may hold values from -0.09375 to 0.09375
- up_weight: bfloat16 [8, 4096, 2048], P('ep', None, 'tp'), may hold values from -0.09375 to 0.09375
- down_weight: bfloat16 [8, 2048, 4096], P('ep', 'tp'), may hold values from -0.125 to 0.125
- post_gain: float32 [4096], replicated, may hold values from 0.1 to 1.9
Outputs:
- mixed_heads: bfloat16 [8192, 4096], P('ep', 'tp')
- routed_out: bfloat16 [2048, 4096], P(('ep', 'tp'))
The draws below stay inside these ranges and needn't reach their ends.
Inputs may be any that keep to these rules, and one draw needn't show every extreme that they name: `expert_pick`: each row names 2 different experts, both in the same one of 4 equal groups of consecutive expert numbers. In every aligned block of 64 rows no expert is named more than 32 times, and some expert exactly 32 times.
All inputs are finite; a program needn't handle non-finite values.
Results may differ from the reference program's by a relative error of at most 0.015.
Values may be sent and summed in bfloat16 or wider, within the bound.
A program may use at most 128 MiB of HBM per device.

```python
import math
import jax
import jax.numpy as jnp
from jax import lax

D = 4096
HEADS = 16
DK = 128
DV = 256
FF = 2048
GROUPS = 4
TOP_K = 2
BLK = 64
TOK_A_DEV = 1024
SPAN_LENGTH = 8192
TOK_B = 2048
EXPERTS = 8
PART_ROWS = 64
CAP = 32
N_EP = 8
N_TP = 4


def draw_decay_logit(key, part):
    channel_count = HEADS * DK
    random_subkeys = jax.random.split(jax.random.fold_in(key, 7), 7)
    slow_level = jnp.log(SPAN_LENGTH * 1.18 / 8.0)
    fast_share = 0.5
    jitter = jax.random.uniform(random_subkeys[0], (SPAN_LENGTH, channel_count), jnp.float32, -1.0, 1.0)
    fast_mask = jax.random.uniform(random_subkeys[1], (channel_count,), jnp.float32) < fast_share
    fast_level = jax.random.uniform(random_subkeys[2], (channel_count,), jnp.float32, 0.5, 1.5)
    slow_spread = jax.random.uniform(random_subkeys[3], (channel_count,), jnp.float32, -0.5, 0.5)
    baseline = jnp.where(fast_mask, fast_level, slow_level + slow_spread)
    shards = SPAN_LENGTH // TOK_A_DEV
    shifts = jax.random.uniform(random_subkeys[4], (shards,), jnp.float32, -0.7, 0.7)
    shift_rows = jnp.repeat(shifts, TOK_A_DEV)
    surge_rows = jax.random.randint(random_subkeys[5], (3,), 0, SPAN_LENGTH)
    surge_value = jax.random.uniform(random_subkeys[6], (3, channel_count), jnp.float32, -11.0, -3.5)
    dropped_indicator = (jnp.arange(SPAN_LENGTH)[:, None] == surge_rows[None, :]).astype(jnp.float32)
    spike_segment = jnp.dot(dropped_indicator, surge_value, precision=lax.Precision.HIGHEST)
    spike_exists = jnp.sum(dropped_indicator, axis=1, keepdims=True) > 0.0
    expert_affinity_scores = baseline[None, :] + jitter + shift_rows[:, None]
    expert_affinity_scores = jnp.where(spike_exists, spike_segment, expert_affinity_scores)
    return jnp.clip(expert_affinity_scores, -11.0, 16.0).astype(jnp.float32)


def pick_block(block_key):
    per_group = EXPERTS // GROUPS
    half_cap = CAP // 2
    random_subkeys = jax.random.split(block_key, 6)
    orders = jax.vmap(lambda one_key: jax.random.permutation(one_key, per_group))(jax.random.split(random_subkeys[0], GROUPS))
    orders = orders.astype(jnp.int32)
    inverse = jnp.argsort(orders, axis=1).astype(jnp.int32)
    offsets = jax.random.randint(random_subkeys[1], (GROUPS, 1), 1, per_group)
    opening_round = jnp.take_along_axis(orders, (inverse + 1) % per_group, axis=1)
    second_turn = jnp.take_along_axis(orders, (inverse + offsets) % per_group, axis=1)
    member = jnp.arange(per_group, dtype=jnp.int32)[None, :, None]
    copy_index = jnp.arange(half_cap, dtype=jnp.int32)[None, None, :]
    partner = jnp.where(copy_index % 2 == 0, opening_round[:, :, None], second_turn[:, :, None])
    group_base = (jnp.arange(GROUPS, dtype=jnp.int32) * per_group)[:, None, None]
    leader = jnp.broadcast_to(group_base + member, partner.shape).reshape(-1)
    follower = (group_base + partner).reshape(-1)
    pair_count = leader.shape[0]
    chosen = jax.random.randint(random_subkeys[2], (), 0, EXPERTS)
    forced = ((leader == chosen) | (follower == chosen)).astype(jnp.int32)
    ranks = jax.random.permutation(random_subkeys[3], pair_count).astype(jnp.int32)
    picked = jnp.argsort(-(ranks + forced * pair_count))[:PART_ROWS]
    picked = picked[jax.random.permutation(random_subkeys[4], PART_ROWS)]
    flips = jax.random.randint(random_subkeys[5], (PART_ROWS,), 0, 2)
    first_col = jnp.where(flips == 1, follower[picked], leader[picked])
    second_col = jnp.where(flips == 1, leader[picked], follower[picked])
    return jnp.stack([first_col, second_col], axis=1).astype(jnp.int32)


def draw_expert_pick(key, part):
    blocks = TOK_B // PART_ROWS
    block_keys = jax.random.split(jax.random.fold_in(key, 11), blocks)
    return jax.vmap(pick_block)(block_keys).reshape(TOK_B, TOP_K).astype(jnp.int32)


def block_scale(stream_key, extent, cuts, least, top_value):
    def one(dim, shards_of):
        steps = jax.random.uniform(jax.random.fold_in(jax.random.fold_in(stream_key, 6), dim), (shards_of,), jnp.float32, least / len(cuts), top_value / len(cuts))
        return jnp.repeat(jnp.exp(steps), extent[dim] // shards_of).reshape((-1,) + (1,) * (len(extent) - dim - 1))

    loudness = one(*cuts[0])
    for cut in cuts[1:]:
        loudness = loudness * one(*cut)
    return loudness


def bell_draw(own_key, dims, deviation, reach, pieces=(), kind=jnp.bfloat16):
    factor_of = block_scale(own_key, dims, pieces, -0.22, 0.18) if pieces else 1.0
    drawn = jax.random.normal(own_key, dims, jnp.float32) * deviation * factor_of
    return jnp.minimum(jnp.maximum(drawn, -reach), reach).astype(kind)


def setup_inputs(seed: int = 0) -> dict:
    streams_of = jax.random.split(jax.random.key(seed), 14)
    return {
        "queries": bell_draw(streams_of[0], (SPAN_LENGTH, HEADS * DK), 1.0, 6.0, ((0, 8), (1, 4))),
        "key_vectors": bell_draw(streams_of[1], (SPAN_LENGTH, HEADS * DK), 1.0, 6.0, ((0, 8), (1, 4))),
        "value_vectors": bell_draw(streams_of[2], (SPAN_LENGTH, HEADS * DV), 1.0, 6.0, ((0, 8), (1, 4))),
        "decay_logit": draw_decay_logit(jax.random.fold_in(streams_of[13], 71), 0),
        "head_gain": jnp.clip(1.0 + 0.18 * jax.random.normal(streams_of[4], (DV,), jnp.float32), 0.1, 1.9),
        "routed_rows": bell_draw(streams_of[5], (TOK_B, D), 1.0, 6.0, ((0, 8),)),
        "pre_gain": jnp.clip(1.0 + 0.18 * jax.random.normal(streams_of[6], (D,), jnp.float32), 0.1, 1.9),
        "expert_pick": draw_expert_pick(jax.random.fold_in(streams_of[13], 71), 0),
        "route_weight": jnp.clip(jnp.exp(math.log(1.0) - 1.609438 * jax.random.uniform(streams_of[8], (TOK_B, TOP_K), jnp.float32) ** block_scale(streams_of[8], (TOK_B, TOP_K), ((0, 8),), -0.2, 0.2)), 0.2, 1.0),
        "gate_weight": bell_draw(streams_of[9], (EXPERTS, D, FF), D ** -0.5, 0.09375, ((0, 8), (2, 4))),
        "up_weight": bell_draw(streams_of[10], (EXPERTS, D, FF), D ** -0.5, 0.09375, ((0, 8), (2, 4))),
        "down_weight": bell_draw(streams_of[11], (EXPERTS, FF, D), FF ** -0.5, 0.125, ((0, 8), (1, 4))),
        "post_gain": jnp.clip(1.0 + 0.18 * jax.random.normal(streams_of[12], (D,), jnp.float32), 0.1, 1.9),
    }


def to_half(array):
    return lax.optimization_barrier(array.astype(jnp.bfloat16))

def row_norm(values, gain):
    return values * lax.rsqrt(lax.optimization_barrier(jnp.mean(values * values, axis=-1, keepdims=True)) + 1e-06) * gain

def token_mixer(queries, key_vectors, value_vectors, decay_logit, head_gain):
    blocks = SPAN_LENGTH // BLK
    key_shape = (blocks, BLK, HEADS, DK)
    log_rate = (jax.nn.log_sigmoid(decay_logit) / 16.0).reshape(key_shape)
    query_blocks = queries.reshape(key_shape)
    key_blocks = key_vectors.reshape(key_shape)
    value_blocks = value_vectors.reshape(blocks, BLK, HEADS, DV)
    causal_mask = jnp.tril(jnp.ones((BLK, BLK), dtype=bool))

    def advance(carry_state, inputs):
        query_rows, key_rows, value_rows, rate_rows = inputs
        cumulative = jnp.cumsum(rate_rows, axis=0)
        ending = cumulative[-1]
        query_decay = to_half(query_rows.astype(jnp.float32) * jnp.exp(cumulative))
        key_decay = to_half(key_rows.astype(jnp.float32) * jnp.exp(-cumulative))
        key_to_end = to_half(key_rows.astype(jnp.float32) * jnp.exp(ending[None] - cumulative))
        values_wide = value_rows.astype(jnp.float32)
        scores = jnp.einsum('ihd,jhd->hij', query_decay.astype(jnp.float32), key_decay.astype(jnp.float32))
        weights = to_half(jnp.where(causal_mask[None], scores, 0.0))
        inside = jnp.einsum('hij,jhe->ihe', weights.astype(jnp.float32), values_wide)
        state_half = to_half(carry_state).astype(jnp.float32)
        carried = jnp.einsum('ihd,hde->ihe', query_decay.astype(jnp.float32), state_half)
        update = jnp.einsum('jhd,jhe->hde', key_to_end.astype(jnp.float32), values_wide)
        next_state = carry_state * jnp.exp(ending)[:, :, None] + update
        produced = row_norm(inside + carried, head_gain).astype(jnp.bfloat16)
        return (next_state, produced)
    start_state = jnp.zeros((HEADS, DK, DV), jnp.float32)
    _, outputs = lax.scan(advance, start_state, (query_blocks, key_blocks, value_blocks, log_rate))
    return outputs.reshape(SPAN_LENGTH, HEADS * DV)

def routed_experts(routed_rows, pre_gain, expert_pick, route_weight, gate_weight, up_weight, down_weight, post_gain):
    normed = row_norm(routed_rows.astype(jnp.float32), pre_gain).astype(jnp.bfloat16)
    flat_pick = expert_pick.reshape(-1).astype(jnp.int32)
    flat_weight = route_weight.reshape(-1)
    expert_room = N_EP * N_TP * CAP
    slice_width = FF // N_TP

    def per_expert(summed, expert):
        ordering = jnp.argsort((flat_pick != expert).astype(jnp.int32), stable=True)[:expert_room].astype(jnp.int32)
        is_live = flat_pick[ordering] == expert
        row_index = (ordering // TOP_K).astype(jnp.int32)
        inputs = normed[row_index].astype(jnp.float32)
        gate_act = jnp.dot(inputs, gate_weight[expert].astype(jnp.float32), preferred_element_type=jnp.float32)
        up_act = jnp.dot(inputs, up_weight[expert].astype(jnp.float32), preferred_element_type=jnp.float32)
        hidden = to_half(jax.nn.silu(gate_act) * up_act).astype(jnp.float32)
        running = jnp.zeros((expert_room, D), jnp.float32)
        for portion in range(N_TP):
            lower_edge = portion * slice_width
            partial_value = jnp.dot(hidden[:, lower_edge:lower_edge + slice_width], down_weight[expert, lower_edge:lower_edge + slice_width].astype(jnp.float32), preferred_element_type=jnp.float32)
            running = running + to_half(partial_value).astype(jnp.float32)
        produced = to_half(running).astype(jnp.float32)
        factor = jnp.where(is_live, flat_weight[ordering], jnp.zeros_like(flat_weight[ordering]))
        return (summed.at[row_index].add(factor[:, None] * produced), None)
    summed, _ = lax.scan(per_expert, jnp.zeros((TOK_B, D), jnp.float32), jnp.arange(EXPERTS, dtype=jnp.int32))
    return row_norm(summed, post_gain).astype(jnp.bfloat16)

def reference(queries, key_vectors, value_vectors, decay_logit, head_gain, routed_rows, pre_gain, expert_pick, route_weight, gate_weight, up_weight, down_weight, post_gain):
    mixed_heads = token_mixer(queries, key_vectors, value_vectors, decay_logit, head_gain)
    routed_out = routed_experts(routed_rows, pre_gain, expert_pick, route_weight, gate_weight, up_weight, down_weight, post_gain)
    return (mixed_heads, routed_out)
```

```python
import functools

import jax
import jax.numpy as jnp
from jax import lax
from jax.experimental import pallas as pl
from jax.experimental.pallas import tpu as pltpu
from jax.sharding import PartitionSpec as P

DK = 128
DV = 256
BLK = 64
CHUNK = 256
GROUPS = 4


def row_norm(values, gain):
    return values * lax.rsqrt(jnp.mean(values * values, axis=-1, keepdims=True) + 1e-06) * gain


def log_rate_of(logit):
    return (jnp.minimum(logit, 0.0) - jnp.log1p(jnp.exp(-jnp.abs(logit)))) * (1.0 / 16.0)


def ordered_sum(mask, values):
    return jnp.dot(
        mask.astype(jnp.float32),
        values,
        precision=lax.Precision.HIGHEST,
        preferred_element_type=jnp.float32,
    )


def summary_kernel(heads, key_ref, value_ref, logit_ref, state_ref, decay_ref, total):
    step = pl.program_id(0)
    rows = key_ref.shape[0]

    @pl.when(step == 0)
    def _():
        state_ref[...] = jnp.zeros_like(state_ref)
        total[...] = jnp.zeros_like(total)

    rate = log_rate_of(logit_ref[...])
    row = lax.broadcasted_iota(jnp.int32, (rows, rows), 0)
    col = lax.broadcasted_iota(jnp.int32, (rows, rows), 1)
    after = ordered_sum(col > row, rate)
    ending = after[0:1] + rate[0:1]
    key_to_end = (key_ref[...].astype(jnp.float32) * jnp.exp(after)).astype(jnp.bfloat16)
    fall = jnp.exp(ending)
    for head in range(heads):
        keys = slice(head * DK, (head + 1) * DK)
        update = lax.dot_general(
            value_ref[:, head * DV : (head + 1) * DV],
            key_to_end[:, keys],
            (((0,), (0,)), ((), ())),
            preferred_element_type=jnp.float32,
        )
        state_ref[head] = state_ref[head] * fall[:, keys] + update
    total[...] += ending
    decay_ref[...] = jnp.exp(total[...])


def mixer_kernel(
    heads, query_ref, key_ref, value_ref, logit_ref, start_ref, gain_ref, out_ref, state
):
    @pl.when(pl.program_id(0) == 0)
    def _():
        state[...] = start_ref[...]

    rows = key_ref.shape[0]
    rate = log_rate_of(logit_ref[...])
    row = lax.broadcasted_iota(jnp.int32, (rows, rows), 0)
    col = lax.broadcasted_iota(jnp.int32, (rows, rows), 1)
    cumulative = ordered_sum((col <= row) & (col // BLK == row // BLK), rate)
    query_decay = (query_ref[...].astype(jnp.float32) * jnp.exp(cumulative)).astype(jnp.bfloat16)
    keys_wide = key_ref[...].astype(jnp.float32)
    key_decay = (keys_wide * jnp.exp(-cumulative)).astype(jnp.bfloat16)
    causal = lax.broadcasted_iota(jnp.int32, (BLK, BLK), 1) <= lax.broadcasted_iota(
        jnp.int32, (BLK, BLK), 0
    )
    gain = gain_ref[...]
    for block in range(rows // BLK):
        here = slice(block * BLK, (block + 1) * BLK)
        part = cumulative[here]
        ending = part[BLK - 1 : BLK]
        key_to_end = (keys_wide[here] * jnp.exp(ending - part)).astype(jnp.bfloat16)
        fall = jnp.exp(ending)
        for head in range(heads):
            keys = slice(head * DK, (head + 1) * DK)
            values = value_ref[here, head * DV : (head + 1) * DV]
            scores = lax.dot_general(
                query_decay[here, keys],
                key_decay[here, keys],
                (((1,), (1,)), ((), ())),
                preferred_element_type=jnp.float32,
            )
            weights = jnp.where(causal, scores, 0.0).astype(jnp.bfloat16)
            inside = jnp.dot(weights, values, preferred_element_type=jnp.float32)
            before = state[head]
            carried = lax.dot_general(
                query_decay[here, keys],
                before.astype(jnp.bfloat16),
                (((1,), (1,)), ((), ())),
                preferred_element_type=jnp.float32,
            )
            update = lax.dot_general(
                values,
                key_to_end[:, keys],
                (((0,), (0,)), ((), ())),
                preferred_element_type=jnp.float32,
            )
            state[head] = before * fall[:, keys] + update
            out_ref[here, head * DV : (head + 1) * DV] = row_norm(inside + carried, gain).astype(
                out_ref.dtype
            )


def entering(decay, state):
    ep_count = lax.axis_size("ep")
    place = lax.axis_index("ep")

    def from_earlier(value, distance):
        pairs = [(i, i + distance) for i in range(ep_count - distance)]
        return lax.ppermute(value, "ep", pairs)

    def moved(pair, distance):
        fall, held = pair
        fall = from_earlier(fall.astype(jnp.bfloat16), distance).astype(jnp.float32)
        held = from_earlier(held.astype(jnp.bfloat16), distance).astype(jnp.float32)
        return (jnp.where(place >= distance, fall, 1.0), held)

    def join(earlier, later):
        return (earlier[0] * later[0], earlier[1] * later[0][:, None, :] + later[1])

    own = (decay, state)
    window = moved(own, 1)
    distance = 2
    while distance < ep_count:
        window = join(moved(join(window, own), distance), window)
        distance *= 2
    return window[1]


def token_mixer(queries, key_vectors, value_vectors, decay_logit, head_gain):
    positions = queries.shape[0]
    heads = queries.shape[1] // DK
    chunk = CHUNK if positions % CHUNK == 0 else BLK
    steps = positions // chunk

    def rows_of(width):
        return pl.BlockSpec((chunk, width), lambda n: (n, 0))

    def whole(shape):
        return pl.BlockSpec(shape, lambda n: (0,) * len(shape))

    key_width, value_width = heads * DK, heads * DV
    order = pltpu.CompilerParams(dimension_semantics=("arbitrary",))
    state, decay = pl.pallas_call(
        functools.partial(summary_kernel, heads),
        grid=(steps,),
        in_specs=[rows_of(key_width), rows_of(value_width), rows_of(key_width)],
        out_specs=[whole((heads, DV, DK)), whole((1, key_width))],
        out_shape=[
            jax.ShapeDtypeStruct((heads, DV, DK), jnp.float32),
            jax.ShapeDtypeStruct((1, key_width), jnp.float32),
        ],
        scratch_shapes=[pltpu.VMEM((1, key_width), jnp.float32)],
        compiler_params=order,
        cost_estimate=pl.CostEstimate(
            flops=4000000000, bytes_accessed=positions * heads * 1280, transcendentals=2000000
        ),
        name="summary",
    )(key_vectors, value_vectors, decay_logit)
    start = entering(decay.reshape(heads, DK), state)
    return pl.pallas_call(
        functools.partial(mixer_kernel, heads),
        grid=(steps,),
        in_specs=[
            rows_of(key_width),
            rows_of(key_width),
            rows_of(value_width),
            rows_of(key_width),
            whole((heads, DV, DK)),
            whole((1, DV)),
        ],
        out_specs=rows_of(value_width),
        out_shape=jax.ShapeDtypeStruct((positions, value_width), jnp.bfloat16),
        scratch_shapes=[pltpu.VMEM((heads, DV, DK), jnp.float32)],
        compiler_params=order,
        cost_estimate=pl.CostEstimate(
            flops=16000000000, bytes_accessed=positions * heads * 2048, transcendentals=4000000
        ),
        name="mixer",
    )(queries, key_vectors, value_vectors, decay_logit, start, head_gain.reshape(1, DV))


def routed_pairs(
    routed_rows, pre_gain, expert_pick, route_weight, gate_weight, up_weight, down_weight, post_gain
):
    tp_count = lax.axis_size("tp")
    ep_count = lax.axis_size("ep")
    part_index = lax.axis_index("tp")
    place = lax.axis_index("ep")
    ep_rows, width = routed_rows.shape
    part_rows = ep_rows // tp_count
    top_count = expert_pick.shape[1]
    members = ep_count // GROUPS
    room = 2 * top_count * part_rows // ep_count
    along = [[m + g * members for g in range(GROUPS)] for m in range(members)]
    plane_size = members * tp_count
    planes = [[g * plane_size + i for i in range(plane_size)] for g in range(GROUPS)]
    my_group = place // members

    own_rows = lax.dynamic_slice_in_dim(routed_rows, part_index * part_rows, part_rows, 0)
    normed = row_norm(own_rows.astype(jnp.float32), pre_gain).astype(jnp.bfloat16)
    seen = lax.all_gather(normed, "ep", axis_index_groups=along)

    notes = jnp.concatenate([expert_pick.astype(jnp.float32).T, route_weight.T], axis=0)
    notes = lax.all_gather(notes, "ep").reshape(
        GROUPS, members, 2 * top_count, tp_count, part_rows
    )
    notes = notes.transpose(1, 3, 0, 2, 4)
    picks, shares = notes[..., :top_count, :], notes[..., top_count:, :]
    group_of = jnp.floor(picks[..., 0, :] / members).astype(jnp.int32)

    def slots_of(mine):
        order = jnp.cumsum(mine.astype(jnp.int32), axis=-1) - 1
        slot = jnp.arange(room, dtype=jnp.int32)[:, None]
        return mine[..., None, :] & (order[..., None, :] == slot)

    table = slots_of(group_of == my_group)
    share = jnp.sum(jnp.where(picks == place.astype(jnp.float32), shares, 0.0), axis=-2)
    slot_share = jnp.sum(jnp.where(table, share[..., None, :], 0.0), axis=-1).reshape(-1, 1)

    own_table = lax.dynamic_index_in_dim(
        lax.dynamic_index_in_dim(table, place % members, 0, False), part_index, 0, False
    )
    chosen = jnp.einsum(
        "gsr,grd->gsd",
        own_table.astype(jnp.bfloat16),
        seen,
        preferred_element_type=jnp.float32,
    ).astype(jnp.bfloat16)
    arrived = lax.all_gather(
        chosen.reshape(GROUPS * room, width),
        ("ep", "tp"),
        axis_index_groups=planes,
        tiled=True,
    )
    gate_act = jnp.dot(arrived, gate_weight[0], preferred_element_type=jnp.float32)
    up_act = jnp.dot(arrived, up_weight[0], preferred_element_type=jnp.float32)
    hidden = (jax.nn.silu(gate_act) * up_act).astype(jnp.bfloat16)
    product = jnp.dot(hidden, down_weight[0], preferred_element_type=jnp.float32)
    summed = lax.psum_scatter(
        (product * slot_share).astype(jnp.bfloat16),
        ("ep", "tp"),
        scatter_dimension=0,
        axis_index_groups=planes,
        tiled=True,
    )
    returned = lax.all_to_all(
        summed.reshape(GROUPS, room, width),
        "ep",
        split_axis=0,
        concat_axis=0,
        axis_index_groups=along,
        tiled=True,
    )
    own_picks = lax.dynamic_slice_in_dim(expert_pick, part_index * part_rows, part_rows, 0)
    own_group = own_picks[:, 0] // members
    places = slots_of(own_group[None, :] == jnp.arange(GROUPS, dtype=jnp.int32)[:, None])
    combined = jnp.einsum(
        "gsr,gsd->rd", places.astype(jnp.bfloat16), returned, preferred_element_type=jnp.float32
    )
    return row_norm(combined, post_gain).astype(jnp.bfloat16)


def routed_any(
    routed_rows, pre_gain, expert_pick, route_weight, gate_weight, up_weight, down_weight, post_gain
):
    tp_count = lax.axis_size("tp")
    ep_count = lax.axis_size("ep")
    part_index = lax.axis_index("tp")
    ep_rows, model_width = routed_rows.shape
    part_rows = ep_rows // tp_count
    top_count = expert_pick.shape[1]
    experts = ep_count * gate_weight.shape[0]
    capacity = 2 * top_count * part_rows // experts
    normed = row_norm(routed_rows.astype(jnp.float32), pre_gain).astype(jnp.bfloat16)
    padded = jnp.concatenate([normed, jnp.zeros((1, model_width), jnp.bfloat16)], axis=0)
    picks = expert_pick.reshape(tp_count, part_rows * top_count)
    matches = (picks[:, :, None] == jnp.arange(experts, dtype=jnp.int32)[None, None, :]).astype(
        jnp.int32
    )
    slots = jnp.sum((jnp.cumsum(matches, axis=1) - 1) * matches, axis=2)
    targets = picks * capacity + slots
    sources = (
        jnp.arange(part_rows * top_count, dtype=jnp.int32)[None, :] // top_count
        + part_rows * jnp.arange(tp_count, dtype=jnp.int32)[:, None]
    )
    slice_offset_index = jnp.broadcast_to(
        jnp.arange(tp_count, dtype=jnp.int32)[:, None], targets.shape
    )
    table = (
        jnp.full((tp_count, experts * capacity), ep_rows, jnp.int32)
        .at[slice_offset_index, targets]
        .set(sources)
    )
    gate_local = gate_weight[0]
    up_local = up_weight[0]
    down_local = down_weight[0]
    own_table = lax.dynamic_slice_in_dim(table, part_index, 1, 0)
    outgoing = padded[own_table].reshape(1, ep_count, capacity, model_width)
    arrived = lax.all_gather(
        lax.all_to_all(outgoing, "ep", split_axis=1, concat_axis=1, tiled=True),
        "tp",
        axis=0,
        tiled=True,
    )
    gate_act = jnp.einsum("pskd,df->pskf", arrived, gate_local, preferred_element_type=jnp.float32)
    up_act = jnp.einsum("pskd,df->pskf", arrived, up_local, preferred_element_type=jnp.float32)
    hidden = (jax.nn.silu(gate_act) * up_act).astype(jnp.bfloat16)
    summed = lax.psum_scatter(
        jnp.einsum("pskf,fd->pskd", hidden, down_local, preferred_element_type=jnp.float32).astype(
            jnp.bfloat16
        ),
        "tp",
        scatter_dimension=0,
        tiled=True,
    )
    returned = lax.all_to_all(summed, "ep", split_axis=1, concat_axis=1, tiled=True)
    flattened = returned.reshape(experts * capacity, model_width)
    my_slots = lax.dynamic_slice_in_dim(targets, part_index, 1, 0).reshape(part_rows, top_count)
    my_weight = lax.dynamic_slice_in_dim(route_weight, part_index * part_rows, part_rows, 0)
    combined = jnp.sum(flattened[my_slots].astype(jnp.float32) * my_weight[:, :, None], axis=1)
    return row_norm(combined, post_gain).astype(jnp.bfloat16)


def routed_experts(
    routed_rows, pre_gain, expert_pick, route_weight, gate_weight, up_weight, down_weight, post_gain
):
    whole_groups = lax.axis_size("ep") == GROUPS * expert_pick.shape[1]
    form = routed_pairs if whole_groups and gate_weight.shape[0] == 1 else routed_any
    return form(
        routed_rows,
        pre_gain,
        expert_pick,
        route_weight,
        gate_weight,
        up_weight,
        down_weight,
        post_gain,
    )


def on_device(
    queries,
    key_vectors,
    value_vectors,
    decay_logit,
    head_gain,
    routed_rows,
    pre_gain,
    expert_pick,
    route_weight,
    gate_weight,
    up_weight,
    down_weight,
    post_gain,
):
    mixed_heads = token_mixer(queries, key_vectors, value_vectors, decay_logit, head_gain)
    routed_out = routed_experts(
        routed_rows,
        pre_gain,
        expert_pick,
        route_weight,
        gate_weight,
        up_weight,
        down_weight,
        post_gain,
    )
    return (mixed_heads, routed_out)


def solution(mesh):
    placed = (
        P("ep", "tp"),
        P("ep", "tp"),
        P("ep", "tp"),
        P("ep", "tp"),
        P(),
        P("ep", None),
        P(),
        P("ep", None),
        P("ep", None),
        P("ep", None, "tp"),
        P("ep", None, "tp"),
        P("ep", "tp", None),
        P(),
    )
    return jax.shard_map(
        on_device,
        mesh=mesh,
        in_specs=placed,
        out_specs=(P("ep", "tp"), P(("ep", "tp"), None)),
        check_vma=False,
    )
```

```python
import functools

import jax
import jax.numpy as jnp
from jax import lax
from jax.experimental import pallas as pl
from jax.experimental.pallas import tpu as pltpu
from jax.sharding import PartitionSpec as P

DK = 128
DV = 256
BLK = 64
CHUNK = 256
GROUPS = 4


def row_norm(values, gain):
    return values * lax.rsqrt(jnp.mean(values * values, axis=-1, keepdims=True) + 1e-06) * gain


def log_rate_of(logit):
    return (jnp.minimum(logit, 0.0) - jnp.log1p(jnp.exp(-jnp.abs(logit)))) * (1.0 / 16.0)


def ordered_sum(mask, values):
    return jnp.dot(
        mask.astype(jnp.float32),
        values,
        precision=lax.Precision.HIGHEST,
        preferred_element_type=jnp.float32,
    )


def summary_kernel(heads, key_ref, value_ref, logit_ref, state_ref, decay_ref, total):
    step = pl.program_id(0)
    rows = key_ref.shape[0]

    @pl.when(step == 0)
    def _():
        state_ref[...] = jnp.zeros_like(state_ref)
        total[...] = jnp.zeros_like(total)

    rate = log_rate_of(logit_ref[...])
    row = lax.broadcasted_iota(jnp.int32, (rows, rows), 0)
    col = lax.broadcasted_iota(jnp.int32, (rows, rows), 1)
    after = ordered_sum(col > row, rate)
    ending = after[0:1] + rate[0:1]
    key_to_end = (key_ref[...].astype(jnp.float32) * jnp.exp(after)).astype(jnp.bfloat16)
    fall = jnp.exp(ending)
    for head in range(heads):
        keys = slice(head * DK, (head + 1) * DK)
        update = lax.dot_general(
            value_ref[:, head * DV : (head + 1) * DV],
            key_to_end[:, keys],
            (((0,), (0,)), ((), ())),
            preferred_element_type=jnp.float32,
        )
        state_ref[head] = state_ref[head] * fall[:, keys] + update
    total[...] += ending
    decay_ref[...] = jnp.exp(total[...])


def mixer_kernel(
    heads, query_ref, key_ref, value_ref, logit_ref, start_ref, gain_ref, out_ref, state
):
    @pl.when(pl.program_id(0) == 0)
    def _():
        state[...] = start_ref[...]

    rows = key_ref.shape[0]
    rate = log_rate_of(logit_ref[...])
    row = lax.broadcasted_iota(jnp.int32, (rows, rows), 0)
    col = lax.broadcasted_iota(jnp.int32, (rows, rows), 1)
    cumulative = ordered_sum((col <= row) & (col // BLK == row // BLK), rate)
    query_decay = (query_ref[...].astype(jnp.float32) * jnp.exp(cumulative)).astype(jnp.bfloat16)
    keys_wide = key_ref[...].astype(jnp.float32)
    key_decay = (keys_wide * jnp.exp(-cumulative)).astype(jnp.bfloat16)
    causal = lax.broadcasted_iota(jnp.int32, (BLK, BLK), 1) <= lax.broadcasted_iota(
        jnp.int32, (BLK, BLK), 0
    )
    gain = gain_ref[...]
    for block in range(rows // BLK):
        here = slice(block * BLK, (block + 1) * BLK)
        part = cumulative[here]
        ending = part[BLK - 1 : BLK]
        key_to_end = (keys_wide[here] * jnp.exp(ending - part)).astype(jnp.bfloat16)
        fall = jnp.exp(ending)
        for head in range(heads):
            keys = slice(head * DK, (head + 1) * DK)
            values = value_ref[here, head * DV : (head + 1) * DV]
            scores = lax.dot_general(
                query_decay[here, keys],
                key_decay[here, keys],
                (((1,), (1,)), ((), ())),
                preferred_element_type=jnp.float32,
            )
            weights = jnp.where(causal, scores, 0.0).astype(jnp.bfloat16)
            inside = jnp.dot(weights, values, preferred_element_type=jnp.float32)
            before = state[head]
            carried = lax.dot_general(
                query_decay[here, keys],
                before.astype(jnp.bfloat16),
                (((1,), (1,)), ((), ())),
                preferred_element_type=jnp.float32,
            )
            update = lax.dot_general(
                values,
                key_to_end[:, keys],
                (((0,), (0,)), ((), ())),
                preferred_element_type=jnp.float32,
            )
            state[head] = before * fall[:, keys] + update
            out_ref[here, head * DV : (head + 1) * DV] = row_norm(inside + carried, gain).astype(
                out_ref.dtype
            )


def entering(decay, state):
    ep_count = lax.axis_size("ep")
    place = lax.axis_index("ep")

    def from_earlier(value, distance):
        pairs = [(i, i + distance) for i in range(ep_count - distance)]
        return lax.ppermute(value, "ep", pairs)

    def moved(pair, distance):
        fall, held = pair
        fall = from_earlier(fall.astype(jnp.bfloat16), distance).astype(jnp.float32)
        held = from_earlier(held.astype(jnp.bfloat16), distance).astype(jnp.float32)
        return (jnp.where(place >= distance, fall, 1.0), held)

    def join(earlier, later):
        return (earlier[0] * later[0], earlier[1] * later[0][:, None, :] + later[1])

    own = (decay, state)
    window = moved(own, 1)
    distance = 2
    while distance < ep_count:
        window = join(moved(join(window, own), distance), window)
        distance *= 2
    return window[1]


def rows_of(chunk, width):
    return pl.BlockSpec((chunk, width), lambda n: (n, 0))


def whole(shape):
    return pl.BlockSpec(shape, lambda n: (0,) * len(shape))


def sizes_of(keys):
    positions, key_width = keys.shape
    heads = key_width // DK
    chunk = CHUNK if positions % CHUNK == 0 else BLK
    return positions, heads, chunk, key_width, heads * DV


ORDER = pltpu.CompilerParams(dimension_semantics=("arbitrary",))


def starting_state(key_vectors, value_vectors, decay_logit):
    positions, heads, chunk, key_width, value_width = sizes_of(key_vectors)
    state, decay = pl.pallas_call(
        functools.partial(summary_kernel, heads),
        grid=(positions // chunk,),
        in_specs=[rows_of(chunk, key_width), rows_of(chunk, value_width), rows_of(chunk, key_width)],
        out_specs=[whole((heads, DV, DK)), whole((1, key_width))],
        out_shape=[
            jax.ShapeDtypeStruct((heads, DV, DK), jnp.float32),
            jax.ShapeDtypeStruct((1, key_width), jnp.float32),
        ],
        scratch_shapes=[pltpu.VMEM((1, key_width), jnp.float32)],
        compiler_params=ORDER,
        cost_estimate=pl.CostEstimate(
            flops=4000000000, bytes_accessed=positions * heads * 1280, transcendentals=2000000
        ),
        name="summary",
    )(key_vectors, value_vectors, decay_logit)
    return entering(decay.reshape(heads, DK), state)


def token_mixer(queries, key_vectors, value_vectors, decay_logit, head_gain, start):
    positions, heads, chunk, key_width, value_width = sizes_of(queries)
    return pl.pallas_call(
        functools.partial(mixer_kernel, heads),
        grid=(positions // chunk,),
        in_specs=[
            rows_of(chunk, key_width),
            rows_of(chunk, key_width),
            rows_of(chunk, value_width),
            rows_of(chunk, key_width),
            whole((heads, DV, DK)),
            whole((1, DV)),
        ],
        out_specs=rows_of(chunk, value_width),
        out_shape=jax.ShapeDtypeStruct((positions, value_width), jnp.bfloat16),
        scratch_shapes=[pltpu.VMEM((heads, DV, DK), jnp.float32)],
        compiler_params=ORDER,
        cost_estimate=pl.CostEstimate(
            flops=16000000000, bytes_accessed=positions * heads * 2048, transcendentals=4000000
        ),
        name="mixer",
    )(queries, key_vectors, value_vectors, decay_logit, start, head_gain.reshape(1, DV))


def routed_pairs(
    routed_rows,
    pre_gain,
    expert_pick,
    route_weight,
    gate_weight,
    up_weight,
    down_weight,
    post_gain,
    start,
):
    tp_count = lax.axis_size("tp")
    ep_count = lax.axis_size("ep")
    part_index = lax.axis_index("tp")
    place = lax.axis_index("ep")
    ep_rows, width = routed_rows.shape
    part_rows = ep_rows // tp_count
    top_count = expert_pick.shape[1]
    members = ep_count // GROUPS
    room = 2 * top_count * part_rows // ep_count
    along = [[m + g * members for g in range(GROUPS)] for m in range(members)]
    plane_size = members * tp_count
    planes = [[g * plane_size + i for i in range(plane_size)] for g in range(GROUPS)]
    my_group = place // members

    own_rows = lax.dynamic_slice_in_dim(routed_rows, part_index * part_rows, part_rows, 0)
    normed = row_norm(own_rows.astype(jnp.float32), pre_gain).astype(jnp.bfloat16)

    notes = jnp.concatenate([expert_pick.astype(jnp.float32).T, route_weight.T], axis=0)
    notes = lax.all_gather(notes, "ep").reshape(
        GROUPS, members, 2 * top_count, tp_count, part_rows
    )
    notes = notes.transpose(1, 3, 0, 2, 4)
    picks, shares = notes[..., :top_count, :], notes[..., top_count:, :]
    group_of = jnp.floor(picks[..., 0, :] / members).astype(jnp.int32)

    def slots_of(mine):
        order = jnp.cumsum(mine.astype(jnp.int32), axis=-1) - 1
        slot = jnp.arange(room, dtype=jnp.int32)[:, None]
        return mine[..., None, :] & (order[..., None, :] == slot)

    table = slots_of(group_of == my_group)
    share = jnp.sum(jnp.where(picks == place.astype(jnp.float32), shares, 0.0), axis=-2)
    slot_share = jnp.sum(jnp.where(table, share[..., None, :], 0.0), axis=-1)

    own_picks = lax.dynamic_slice_in_dim(expert_pick, part_index * part_rows, part_rows, 0)
    own_group = own_picks[:, 0] // members
    places = slots_of(own_group[None, :] == jnp.arange(GROUPS, dtype=jnp.int32)[:, None]).astype(
        jnp.bfloat16
    )
    leaving = jnp.einsum(
        "gsr,rd->gsd", places, normed, preferred_element_type=jnp.float32
    ).astype(jnp.bfloat16)
    chosen = lax.all_to_all(
        leaving, "ep", split_axis=0, concat_axis=0, axis_index_groups=along, tiled=True
    )
    spans = 2 if room % 16 == 0 else 1
    span = room // spans
    slot_share = slot_share.reshape(plane_size, GROUPS, spans, span)

    def gathered(turn):
        return lax.all_gather(
            chosen[:, turn * span : (turn + 1) * span].reshape(GROUPS * span, width),
            ("ep", "tp"),
            axis_index_groups=planes,
            tiled=True,
        )

    def experts_on(arrived, turn):
        gate_act = jnp.dot(arrived, gate_weight[0], preferred_element_type=jnp.float32)
        up_act = jnp.dot(arrived, up_weight[0], preferred_element_type=jnp.float32)
        hidden = (jax.nn.silu(gate_act) * up_act).astype(jnp.bfloat16)
        product = jnp.dot(hidden, down_weight[0], preferred_element_type=jnp.float32)
        return (product * slot_share[:, :, turn].reshape(-1, 1)).astype(jnp.bfloat16)

    def sent_home(product):
        summed = lax.psum_scatter(
            product,
            ("ep", "tp"),
            scatter_dimension=0,
            axis_index_groups=planes,
            tiled=True,
        )
        return lax.all_to_all(
            summed.reshape(GROUPS, span, width),
            "ep",
            split_axis=0,
            concat_axis=0,
            axis_index_groups=along,
            tiled=True,
        )

    arrivals = [gathered(turn) for turn in range(spans)]
    arrivals[0], start = lax.optimization_barrier((arrivals[0], start))
    returned = jnp.concatenate(
        [sent_home(experts_on(arrived, turn)) for turn, arrived in enumerate(arrivals)], axis=1
    )
    combined = jnp.einsum(
        "gsr,gsd->rd", places, returned, preferred_element_type=jnp.float32
    )
    return (row_norm(combined, post_gain).astype(jnp.bfloat16), start)


def routed_any(
    routed_rows, pre_gain, expert_pick, route_weight, gate_weight, up_weight, down_weight, post_gain
):
    tp_count = lax.axis_size("tp")
    ep_count = lax.axis_size("ep")
    part_index = lax.axis_index("tp")
    ep_rows, model_width = routed_rows.shape
    part_rows = ep_rows // tp_count
    top_count = expert_pick.shape[1]
    experts = ep_count * gate_weight.shape[0]
    capacity = 2 * top_count * part_rows // experts
    normed = row_norm(routed_rows.astype(jnp.float32), pre_gain).astype(jnp.bfloat16)
    padded = jnp.concatenate([normed, jnp.zeros((1, model_width), jnp.bfloat16)], axis=0)
    picks = expert_pick.reshape(tp_count, part_rows * top_count)
    matches = (picks[:, :, None] == jnp.arange(experts, dtype=jnp.int32)[None, None, :]).astype(
        jnp.int32
    )
    slots = jnp.sum((jnp.cumsum(matches, axis=1) - 1) * matches, axis=2)
    targets = picks * capacity + slots
    sources = (
        jnp.arange(part_rows * top_count, dtype=jnp.int32)[None, :] // top_count
        + part_rows * jnp.arange(tp_count, dtype=jnp.int32)[:, None]
    )
    slice_offset_index = jnp.broadcast_to(
        jnp.arange(tp_count, dtype=jnp.int32)[:, None], targets.shape
    )
    table = (
        jnp.full((tp_count, experts * capacity), ep_rows, jnp.int32)
        .at[slice_offset_index, targets]
        .set(sources)
    )
    gate_local = gate_weight[0]
    up_local = up_weight[0]
    down_local = down_weight[0]
    own_table = lax.dynamic_slice_in_dim(table, part_index, 1, 0)
    outgoing = padded[own_table].reshape(1, ep_count, capacity, model_width)
    arrived = lax.all_gather(
        lax.all_to_all(outgoing, "ep", split_axis=1, concat_axis=1, tiled=True),
        "tp",
        axis=0,
        tiled=True,
    )
    gate_act = jnp.einsum("pskd,df->pskf", arrived, gate_local, preferred_element_type=jnp.float32)
    up_act = jnp.einsum("pskd,df->pskf", arrived, up_local, preferred_element_type=jnp.float32)
    hidden = (jax.nn.silu(gate_act) * up_act).astype(jnp.bfloat16)
    summed = lax.psum_scatter(
        jnp.einsum("pskf,fd->pskd", hidden, down_local, preferred_element_type=jnp.float32).astype(
            jnp.bfloat16
        ),
        "tp",
        scatter_dimension=0,
        tiled=True,
    )
    returned = lax.all_to_all(summed, "ep", split_axis=1, concat_axis=1, tiled=True)
    flattened = returned.reshape(experts * capacity, model_width)
    my_slots = lax.dynamic_slice_in_dim(targets, part_index, 1, 0).reshape(part_rows, top_count)
    my_weight = lax.dynamic_slice_in_dim(route_weight, part_index * part_rows, part_rows, 0)
    combined = jnp.sum(flattened[my_slots].astype(jnp.float32) * my_weight[:, :, None], axis=1)
    return row_norm(combined, post_gain).astype(jnp.bfloat16)


def routed_experts(*operands, start):
    expert_pick, gate_weight = operands[2], operands[4]
    whole_groups = lax.axis_size("ep") == GROUPS * expert_pick.shape[1]
    if whole_groups and gate_weight.shape[0] == 1:
        return routed_pairs(*operands, start)
    return (routed_any(*operands), start)


def on_device(
    queries,
    key_vectors,
    value_vectors,
    decay_logit,
    head_gain,
    routed_rows,
    pre_gain,
    expert_pick,
    route_weight,
    gate_weight,
    up_weight,
    down_weight,
    post_gain,
):
    start = starting_state(key_vectors, value_vectors, decay_logit)
    routed_out, start = routed_experts(
        routed_rows,
        pre_gain,
        expert_pick,
        route_weight,
        gate_weight,
        up_weight,
        down_weight,
        post_gain,
        start=start,
    )
    mixed_heads = token_mixer(
        queries, key_vectors, value_vectors, decay_logit, head_gain, start
    )
    return (mixed_heads, routed_out)


def solution(mesh):
    placed = (
        P("ep", "tp"),
        P("ep", "tp"),
        P("ep", "tp"),
        P("ep", "tp"),
        P(),
        P("ep", None),
        P(),
        P("ep", None),
        P("ep", None),
        P("ep", None, "tp"),
        P("ep", None, "tp"),
        P("ep", "tp", None),
        P(),
    )
    return jax.shard_map(
        on_device,
        mesh=mesh,
        in_specs=placed,
        out_specs=(P("ep", "tp"), P(("ep", "tp"), None)),
        check_vma=False,
    )
```
